32 devices in a mesh: sp: 16 (over z, y, x), tp: 2 (over core).
Axes of the slice: x: 2, y: 2, z: 4, core: 2. Of those that a mesh axis runs over, the one named last changes fastest.
Arguments:
- tokens: bfloat16 [4096, 2048], P('sp', 'tp'), may hold values from -6 to 6
- outer_gate: bfloat16 [2048, 1024], P(None, 'tp'), may hold values from -0.125 to 0.125
- inner_gate: bfloat16 [2048, 1024], P(None, 'tp'), may hold values from -0.125 to 0.125
- conv_input: bfloat16 [2048, 1024], P(None, 'tp'), may hold values from -0.125 to 0.125
- conv_taps: bfloat16 [3, 1024], P(None, 'tp'), may hold values from -3.5 to 3.5
- query_down: bfloat16 [2048, 512], P(None, 'tp'), may hold values from -0.125 to 0.125
- latent_down: bfloat16 [2048, 256], P(None, 'tp'), may hold values from -0.125 to 0.125
- rotary_down: bfloat16 [2048, 32], replicated, may hold values from -5.303301 to 5.303301
- query_gain: float32 [512], replicated, may hold values from 0.1 to 1.9
- latent_gain: float32 [256], replicated, may hold values from 0.1 to 1.9
- query_up: bfloat16 [512, 1536], P(None, 'tp'), may hold values from -0.52734375 to 0.52734375
- latent_up: bfloat16 [256, 2048], P(None, 'tp'), may hold values from -0.75 to 0.75
- conv_project: bfloat16 [1024, 2048], P('tp'), may hold values from -0.1875 to 0.1875
- attend_project: bfloat16 [1024, 2048], P('tp'), may hold values from -0.1875 to 0.1875
Outputs:
- mixed: bfloat16 [4096, 2048], P(('sp', 'tp'))
The draws below stay inside these ranges and needn't reach their ends.
All inputs are finite; a program needn't handle non-finite values.
Results may differ from the reference program's by a relative error of at most 0.035.
Values may be sent and summed in bfloat16 or wider, within the bound.
A program may use at most 128 MiB of HBM per device.

```python
import math
import jax
import jax.numpy as jnp
from jax import lax

D = 2048
CW = 1024
HEADS = 16
QR = 512
KVR = 256
NOPE = 64
ROPE = 32
VDIM = 64
KSIZE = 3
TOKENS = 4096
N_TP = 2


def draw_rotary_down(key, part):
    base = jnp.clip(jax.random.normal(key, (D, ROPE), jnp.float32), -6.0, 6.0) * D ** (-0.5)
    return base.astype(jnp.bfloat16)


def steps_of(own_key, dims, shards, smallest, high):
    def one(dim, parts):
        draws = jax.random.uniform(jax.random.fold_in(jax.random.fold_in(own_key, 6), dim), (parts,), jnp.float32, smallest / len(shards), high / len(shards))
        return jnp.repeat(jnp.exp(draws), dims[dim] // parts).reshape((-1,) + (1,) * (len(dims) - dim - 1))

    loudness = one(*shards[0])
    for cut in shards[1:]:
        loudness = loudness * one(*cut)
    return loudness


def noise(stream_key, dims, deviation, most, shards=(), held_as=jnp.bfloat16):
    values = deviation * jax.random.normal(stream_key, dims, jnp.float32)
    if shards:
        values = values * steps_of(stream_key, dims, shards, -0.22, 0.18)
    return jnp.clip(values, -most, most).astype(held_as)


def setup_inputs(seed: int = 0) -> dict:
    keys = jax.random.split(jax.random.key(seed), 15)
    tokens = noise(keys[0], (TOKENS, D), 1.0, 6.0, ((0, 16), (1, 2)))
    outer_gate = noise(keys[1], (D, CW), D ** -0.5, 0.125, ((1, 2),))
    inner_gate = noise(keys[2], (D, CW), D ** -0.5, 0.125, ((1, 2),))
    conv_input = noise(keys[3], (D, CW), D ** -0.5, 0.125, ((1, 2),))
    conv_taps = noise(keys[4], (KSIZE, CW), KSIZE ** -0.5, 3.5, ((1, 2),))
    query_down = noise(keys[5], (D, QR), D ** -0.5, 0.125, ((1, 2),))
    latent_down = noise(keys[6], (D, KVR), D ** -0.5, 0.125, ((1, 2),))
    rotary_down = draw_rotary_down(jax.random.fold_in(keys[14], 71), 0)
    query_gain = jnp.clip(1.0 + 0.18 * jax.random.normal(keys[8], (QR,), jnp.float32), 0.1, 1.9)
    latent_gain = jnp.clip(1.0 + 0.18 * jax.random.normal(keys[9], (KVR,), jnp.float32), 0.1, 1.9)
    query_up = noise(keys[10], (QR, HEADS * (NOPE + ROPE)), (2.0 / QR ** 0.5), 0.52734375, ((1, 2),))
    latent_up = noise(keys[11], (KVR, HEADS * (NOPE + VDIM)), (2.0 / KVR ** 0.5), 0.75, ((1, 2),))
    conv_project = noise(keys[12], (CW, D), CW ** -0.5, 0.1875, ((0, 2),))
    attend_project = noise(keys[13], (HEADS * VDIM, D), (HEADS * VDIM) ** -0.5, 0.1875, ((0, 2),))
    return {"tokens": tokens, "outer_gate": outer_gate, "inner_gate": inner_gate, "conv_input": conv_input, "conv_taps": conv_taps, "query_down": query_down, "latent_down": latent_down, "rotary_down": rotary_down, "query_gain": query_gain, "latent_gain": latent_gain, "query_up": query_up, "latent_up": latent_up, "conv_project": conv_project, "attend_project": attend_project}


neg_fill = -1e+30
rotary_base = 10000.0
norm_epsilon = 1e-06

def matmul(left, right):
    return jnp.dot(left, right, preferred_element_type=jnp.float32)

def rotate(values, positions):
    half = values.shape[-1] // 2
    inverse = rotary_base ** (-(jnp.arange(half, dtype=jnp.float32) * 2.0 / (2 * half)))
    angle = positions[:, None] * inverse[None, :]
    if values.ndim == 3:
        angle = angle[:, None, :]
    cosine = jnp.cos(angle)
    sine = jnp.sin(angle)
    first = values[..., :half]
    second = values[..., half:]
    return jnp.concatenate([first * cosine - second * sine, first * sine + second * cosine], -1)

def rms_scale(latent, gain):
    values = lax.optimization_barrier(latent).astype(jnp.float32)
    factor = lax.rsqrt(lax.optimization_barrier(jnp.mean(values * values, -1, keepdims=True)) + norm_epsilon)
    return (values * factor * gain).astype(jnp.bfloat16)

def reference(tokens, outer_gate, inner_gate, conv_input, conv_taps, query_down, latent_down, rotary_down, query_gain, latent_gain, query_up, latent_up, conv_project, attend_project):
    length = tokens.shape[0]
    outer = matmul(tokens, outer_gate)
    inner = matmul(tokens, inner_gate)
    signal = matmul(tokens, conv_input)
    gated = lax.optimization_barrier((inner * signal).astype(jnp.bfloat16)).astype(jnp.float32)
    padded = jnp.pad(gated, ((KSIZE - 1, 0), (0, 0)))
    taps = conv_taps.astype(jnp.float32)
    filtered = padded[0:length] * taps[0]
    for index in range(1, KSIZE):
        filtered = filtered + padded[index:index + length] * taps[index]
    conv_result = (outer * filtered).astype(jnp.bfloat16)
    positions = jnp.arange(length, dtype=jnp.float32)
    query_norm = rms_scale(matmul(tokens, query_down).astype(jnp.bfloat16), query_gain)
    latent_norm = rms_scale(matmul(tokens, latent_down).astype(jnp.bfloat16), latent_gain)
    rotary_key = rotate(matmul(tokens, rotary_down), positions).astype(jnp.bfloat16)
    query_full = matmul(query_norm, query_up).reshape(length, HEADS, NOPE + ROPE)
    query_plain = query_full[..., :NOPE].astype(jnp.bfloat16).astype(jnp.float32)
    query_rot = rotate(query_full[..., NOPE:], positions).astype(jnp.bfloat16).astype(jnp.float32)
    expanded = matmul(latent_norm, latent_up).astype(jnp.bfloat16).reshape(length, HEADS, NOPE + VDIM)
    key_plain = expanded[..., :NOPE].astype(jnp.float32)
    values = expanded[..., NOPE:].astype(jnp.float32)
    key_rot = rotary_key.astype(jnp.float32)
    scale = (NOPE + ROPE) ** (-0.5)
    block = math.gcd(length, 256)
    key_index = jnp.arange(length)

    def one_block(number):
        first = (number * block).astype(jnp.int32)
        plain = lax.dynamic_slice_in_dim(query_plain, first, block, 0)
        turned = lax.dynamic_slice_in_dim(query_rot, first, block, 0)
        scores = jnp.einsum('qhd,khd->hqk', plain, key_plain) + jnp.einsum('qhr,kr->hqk', turned, key_rot)
        scores = scores * scale
        query_index = first + jnp.arange(block)
        visible = key_index[None, :] <= query_index[:, None]
        scores = jnp.where(visible[None], scores, neg_fill)
        rowmax = lax.optimization_barrier(jnp.max(scores, -1, keepdims=True))
        weight = jnp.exp(scores - rowmax)
        total = lax.optimization_barrier(jnp.sum(weight, -1))
        rounded = weight.astype(jnp.bfloat16).astype(jnp.float32)
        summed = jnp.einsum('hqk,khd->qhd', rounded, values)
        return (summed / total.T[:, :, None]).astype(jnp.bfloat16)
    attended = lax.map(one_block, jnp.arange(length // block, dtype=jnp.int32))
    attended = attended.reshape(length, HEADS * VDIM)
    conv_share = CW // N_TP
    head_share = HEADS * VDIM // N_TP
    result = jnp.zeros((length, D), jnp.float32)
    for group in range(N_TP):
        partial_value = matmul(conv_result[:, group * conv_share:(group + 1) * conv_share], conv_project[group * conv_share:(group + 1) * conv_share])
        partial_value = partial_value + matmul(attended[:, group * head_share:(group + 1) * head_share], attend_project[group * head_share:(group + 1) * head_share])
        result = result + lax.optimization_barrier(partial_value.astype(jnp.bfloat16)).astype(jnp.float32)
    return result.astype(jnp.bfloat16)
```

```python
import jax
import jax.numpy as jnp
from jax import lax
from jax.experimental import pallas as pl
from jax.experimental.pallas import tpu as pltpu
from jax.sharding import PartitionSpec as P

NOPE = 64
ROPE = 32
VDIM = 64
LANES = 128
ONES = 16

neg_fill = -1e30
rotary_base = 10000.0
norm_epsilon = 1e-06
log2e = 1.4426950408889634


def shifted(shard, axis, by):
    length = lax.axis_size(axis)
    pairs = [(i, i + by) for i in range(length) if 0 <= i + by < length]
    return lax.ppermute(shard, axis, pairs)


def angles(positions):
    half = ROPE // 2
    inverse = rotary_base ** (-(jnp.arange(half, dtype=jnp.float32) * 2.0 / (2 * half)))
    return positions[:, None] * inverse[None, :]


def rotate(values, positions):
    half = values.shape[-1] // 2
    angle = angles(positions)
    if values.ndim == 3:
        angle = angle[:, None, :]
    cosine = jnp.cos(angle)
    sine = jnp.sin(angle)
    first = values[..., :half]
    second = values[..., half:]
    return jnp.concatenate([first * cosine - second * sine, first * sine + second * cosine], -1)


def rms_scale(latent, gain):
    values = latent.astype(jnp.float32)
    factor = lax.rsqrt(jnp.mean(values * values, -1, keepdims=True) + norm_epsilon)
    return (values * factor * gain).astype(jnp.bfloat16)


def dot(a, b, dims=((1,), (0,))):
    return lax.dot_general(a, b, (dims, ((), ())), preferred_element_type=jnp.float32)


def attend(lat, rot, qx_ref, up_ref, wvt_ref, best_ref, acc_ref, masked):
    heads = qx_ref.shape[0]
    expanded = dot(lat, up_ref[...]).astype(jnp.bfloat16)
    turned = dot(wvt_ref[...], lat, ((1,), (1,))).astype(jnp.bfloat16)
    ones = jnp.ones((ONES, lat.shape[0]), jnp.bfloat16)
    width = NOPE + VDIM
    for h in range(heads):
        key = jnp.concatenate([expanded[:, h * width : (h + 1) * width], rot], 1)
        s = dot(key, qx_ref[h])
        if masked:
            k_at = lax.broadcasted_iota(jnp.int32, s.shape, 0)
            q_at = lax.broadcasted_iota(jnp.int32, s.shape, 1)
            s = jnp.where(k_at <= q_at, s, neg_fill)
        values = jnp.concatenate([turned[h * VDIM : (h + 1) * VDIM], ones], 0)
        top = jnp.max(s, 0, keepdims=True)
        if masked:
            weight = jnp.exp2(s - top).astype(jnp.bfloat16)
            acc_ref[h] = dot(values, weight)
            best_ref[h] = top
        else:
            old = best_ref[h]
            new = jnp.maximum(old, top)
            weight = jnp.exp2(s - new).astype(jnp.bfloat16)
            acc_ref[h] = acc_ref[h] * jnp.exp2(old - new) + dot(values, weight)
            best_ref[h] = new


def attention_kernel(lat_ref, rot_ref, qx_ref, up_ref, wvt_ref, out_ref, best_ref, acc_ref):
    me = lax.axis_index("sp")
    rows = qx_ref.shape[2]

    def block(j, masked):
        at = pl.ds(pl.multiple_of(j * rows, rows), rows)
        attend(lat_ref[at, :], rot_ref[at, :], qx_ref, up_ref, wvt_ref, best_ref, acc_ref, masked)

    block(me, True)

    @pl.loop(0, me)
    def _(j):
        block(j, False)

    for h in range(qx_ref.shape[0]):
        acc = acc_ref[h]
        out_ref[h * VDIM : (h + 1) * VDIM, :] = (acc[:VDIM] / acc[VDIM : VDIM + 1]).astype(jnp.bfloat16)


def local(
    tokens,
    outer_gate,
    inner_gate,
    conv_input,
    conv_taps,
    query_down,
    latent_down,
    rotary_down,
    query_gain,
    latent_gain,
    query_up,
    latent_up,
    conv_project,
    attend_project,
):
    rows = tokens.shape[0]
    heads = query_up.shape[1] // (NOPE + ROPE)
    weights = (outer_gate, inner_gate, conv_input, query_down, latent_down, rotary_down)
    piece = lax.all_gather(tokens, "tp", axis=1, tiled=True)
    outer, inner, signal, query_part, latent_part, rotary_raw = tuple(
        (jnp.dot(piece, weight, preferred_element_type=jnp.float32) for weight in weights)
    )
    query_lat = lax.all_gather(query_part.astype(jnp.bfloat16), "tp", axis=1, tiled=True)
    latent_lat = lax.all_gather(latent_part.astype(jnp.bfloat16), "tp", axis=1, tiled=True)
    gated = (inner * signal).astype(jnp.bfloat16)
    reach = conv_taps.shape[0] - 1
    rim = shifted(gated[rows - reach :], "sp", 1)
    padded = jnp.concatenate([rim, gated], 0).astype(jnp.float32)
    taps = conv_taps.astype(jnp.float32)
    filtered = padded[0:rows] * taps[0]
    for index in range(1, reach + 1):
        filtered = filtered + padded[index : index + rows] * taps[index]
    conv_result = (outer * filtered).astype(jnp.bfloat16)
    positions = (lax.axis_index("sp") * rows + jnp.arange(rows, dtype=jnp.int32)).astype(jnp.float32)
    query_norm = rms_scale(query_lat, query_gain)
    latent_norm = rms_scale(latent_lat, latent_gain)
    rotary_key = rotate(rotary_raw, positions).astype(jnp.bfloat16)
    scale = (NOPE + ROPE) ** (-0.5) * log2e
    query = jnp.dot(query_norm, query_up, preferred_element_type=jnp.float32) * scale
    query = query.reshape(rows, heads, NOPE + ROPE)
    plain = query[..., :NOPE].astype(jnp.bfloat16)
    turned = rotate(query[..., NOPE:], positions).astype(jnp.bfloat16)
    qx = jnp.concatenate(
        [
            plain,
            jnp.zeros((rows, heads, VDIM), jnp.bfloat16),
            turned,
            jnp.zeros((rows, heads, LANES - ROPE), jnp.bfloat16),
        ],
        2,
    ).transpose(1, 2, 0)
    shared = jnp.concatenate([latent_norm, rotary_key], 1)
    shared = lax.all_gather(shared, "sp", axis=0, tiled=True)
    kvr = latent_norm.shape[1]
    keys = shared[:, :kvr]
    rots = jnp.pad(shared[:, kvr:], ((0, 0), (0, LANES - ROPE)))
    wvt = latent_up.reshape(kvr, heads, NOPE + VDIM)[..., NOPE:].reshape(kvr, heads * VDIM).T
    vmem = pl.BlockSpec(memory_space=pltpu.VMEM)
    attended = pl.pallas_call(
        attention_kernel,
        out_shape=jax.ShapeDtypeStruct((heads * VDIM, rows), jnp.bfloat16),
        in_specs=[vmem] * 5,
        out_specs=vmem,
        scratch_shapes=[
            pltpu.VMEM((heads, 1, rows), jnp.float32),
            pltpu.VMEM((heads, VDIM + ONES, rows), jnp.float32),
        ],
        compiler_params=pltpu.CompilerParams(vmem_limit_bytes=48 * 1024 * 1024),
    )(keys, rots, qx, latent_up, wvt)
    partial = jnp.dot(conv_result, conv_project, preferred_element_type=jnp.float32)
    partial = partial + dot(attended, attend_project, ((0,), (0,)))
    return lax.psum_scatter(partial.astype(jnp.bfloat16), "tp", scatter_dimension=0, tiled=True)


def solution(mesh):
    split = P(None, "tp")
    in_specs = (P("sp", "tp"),) + (split,) * 6 + (P(),) * 3 + (split,) * 2 + (P("tp", None),) * 2
    out_specs = P(("sp", "tp"), None)
    return jax.shard_map(local, mesh=mesh, in_specs=in_specs, out_specs=out_specs, check_vma=False)
```

```python
import jax
import jax.numpy as jnp
from jax import lax
from jax.experimental import pallas as pl
from jax.experimental.pallas import tpu as pltpu
from jax.sharding import PartitionSpec as P

NOPE = 64
ROPE = 32
VDIM = 64
LANES = 128
ONES = 16

MESH = pl.DeviceIdType.MESH
neg_fill = -1e30
rotary_base = 10000.0
norm_epsilon = 1e-06
log2e = 1.4426950408889634


def shifted(shard, axis, by):
    length = lax.axis_size(axis)
    pairs = [(i, i + by) for i in range(length) if 0 <= i + by < length]
    return lax.ppermute(shard, axis, pairs)


def angles(positions):
    half = ROPE // 2
    inverse = rotary_base ** (-(jnp.arange(half, dtype=jnp.float32) * 2.0 / (2 * half)))
    return positions[:, None] * inverse[None, :]


def rotate(values, positions):
    half = values.shape[-1] // 2
    angle = angles(positions)
    if values.ndim == 3:
        angle = angle[:, None, :]
    cosine = jnp.cos(angle)
    sine = jnp.sin(angle)
    first = values[..., :half]
    second = values[..., half:]
    return jnp.concatenate([first * cosine - second * sine, first * sine + second * cosine], -1)


def rms_scale(latent, gain):
    values = latent.astype(jnp.float32)
    factor = lax.rsqrt(jnp.mean(values * values, -1, keepdims=True) + norm_epsilon)
    return (values * factor * gain).astype(jnp.bfloat16)


def dot(a, b, dims=((1,), (0,))):
    return lax.dot_general(a, b, (dims, ((), ())), preferred_element_type=jnp.float32)


def attend(lat, rot, qx_ref, up_ref, wvt_ref, best_ref, acc_ref, masked):
    heads = qx_ref.shape[0]
    expanded = dot(lat, up_ref[...]).astype(jnp.bfloat16)
    turned = dot(wvt_ref[...], lat, ((1,), (1,))).astype(jnp.bfloat16)
    ones = jnp.ones((ONES, lat.shape[0]), jnp.bfloat16)
    width = NOPE + VDIM
    for h in range(heads):
        key = jnp.concatenate([expanded[:, h * width : (h + 1) * width], rot], 1)
        s = dot(key, qx_ref[h])
        if masked:
            k_at = lax.broadcasted_iota(jnp.int32, s.shape, 0)
            q_at = lax.broadcasted_iota(jnp.int32, s.shape, 1)
            s = jnp.where(k_at <= q_at, s, neg_fill)
        values = jnp.concatenate([turned[h * VDIM : (h + 1) * VDIM], ones], 0)
        top = jnp.max(s, 0, keepdims=True)
        if masked:
            weight = jnp.exp2(s - top).astype(jnp.bfloat16)
            acc_ref[h] = dot(values, weight)
            best_ref[h] = top
        else:
            old = best_ref[h]
            new = jnp.maximum(old, top)
            weight = jnp.exp2(s - new).astype(jnp.bfloat16)
            acc_ref[h] = acc_ref[h] * jnp.exp2(old - new) + dot(values, weight)
            best_ref[h] = new


def mix_kernel(
    lat_in, rot_in, qx_ref, up_ref, wvt_ref, conv_ref, cproj_ref, aproj_ref, out_ref,
    lat, rot, best_ref, acc_ref, att, part_buf, in_buf,
    own_sem, lat_send, lat_recv, rot_send, rot_recv, share_send, share_recv, tail_send, tail_recv,
):
    me = lax.axis_index("sp")
    t = lax.axis_index("tp")
    total = lax.axis_size("sp")
    ways = lax.axis_size("tp")
    planes = total // 4
    z = me // 4
    b0 = me % 2
    b1 = (me // 2) % 2
    a0 = 1 - t % 2
    rows = qx_ref.shape[2]
    short = rows // ways

    def block_of(plane, ka, kb):
        f0 = a0 * ka + (1 - a0) * kb
        f1 = a0 * kb + (1 - a0) * ka
        return plane * 4 + (b1 + f1 * (1 - 2 * b1)) * 2 + b0 + f0 * (1 - 2 * b0)

    up = lax.rem(me + 4, total)
    down = lax.rem(me + total - 4, total)
    a_peer = block_of(z, 1, 0)
    b_peer = block_of(z, 0, 1)
    mates = [lax.rem(t + o, ways) for o in range(1, ways)]

    barrier = pltpu.get_barrier_semaphore()
    for target in [(up, t), (down, t), (a_peer, t), (b_peer, t)] + [(me, mate) for mate in mates]:
        pl.semaphore_signal(barrier, inc=1, device_id=target, device_id_type=MESH)

    own = [
        pltpu.make_async_copy(lat_in, lat.at[me], own_sem.at[0]),
        pltpu.make_async_copy(rot_in, rot.at[me], own_sem.at[1]),
    ]
    for copy in own:
        copy.start()
    for copy in own:
        copy.wait()
    pl.semaphore_wait(barrier, 4 + len(mates))

    def hop(j, k, target):
        return [
            pltpu.make_async_remote_copy(
                buf.at[j, t] if split else buf.at[j],
                buf.at[j, t] if split else buf.at[j],
                send.at[j, k],
                recv.at[j],
                device_id=(target, t),
                device_id_type=MESH,
            )
            for buf, send, recv, split in ((lat, lat_send, lat_recv, True), (rot, rot_send, rot_recv, False))
        ]

    def start(j, k, target):
        for copy in hop(j, k, target):
            copy.start()

    def arrive(j):
        for copy in hop(j, 0, up):
            copy.wait_recv()

    def shares(j):
        return [
            pltpu.make_async_remote_copy(
                lat.at[j, t],
                lat.at[j, t],
                share_send.at[j, o],
                share_recv.at[j, o],
                device_id=(me, mate),
                device_id_type=MESH,
            )
            for o, mate in enumerate(mates)
        ]

    def share_landed(j):
        for o in range(len(mates)):
            source = lax.rem(t + ways - 1 - o, ways)
            pltpu.make_async_remote_copy(
                lat.at[j, source],
                lat.at[j, source],
                share_send.at[j, o],
                share_recv.at[j, o],
                device_id=(me, mates[o]),
                device_id_type=MESH,
            ).wait_recv()

    def share(j):
        @pl.when(j < me)
        def _():
            for copy in shares(j):
                copy.start()

    def spread(j):
        @pl.when(z + 1 < planes)
        def _():
            start(j, 0, up)

        start(j, 1, a_peer)
        start(j, 2, b_peer)

    def stage_a(d):
        j = block_of(z - d, 0, 0)
        arrive(j)
        spread(j)
        share(j)

    def stage_b(d):
        j = block_of(z - d, 1, 0)
        arrive(j)
        start(j, 2, b_peer)
        share(j)

    def stage_c(d):
        for ka in (0, 1):
            j = block_of(z - d, ka, 1)
            arrive(j)
            share(j)

    def block(j, masked):
        latent = jnp.concatenate([lat[j, s] for s in range(ways)], 1)
        turned = rot[j].astype(jnp.float32)
        turned = jnp.concatenate([turned, jnp.zeros((LANES - ROPE, rows), jnp.float32)], 0)
        turned = turned.T.astype(jnp.bfloat16)
        attend(latent, turned, qx_ref, up_ref, wvt_ref, best_ref, acc_ref, masked)

    spread(me)
    block(me, True)
    stage_b(0)
    stage_c(0)

    @pl.loop(0, 4 * (z + 1))
    def _(n):
        d = n // 4
        k = n % 4
        for order, stage in enumerate((stage_a, stage_b, stage_c)):

            @pl.when(jnp.logical_and(k == order, d < z))
            def _():
                stage(d + 1)

        j = block_of(z - d, k % 2, k // 2)

        @pl.when(j < me)
        def _():
            share_landed(j)
            block(j, False)

    for h in range(qx_ref.shape[0]):
        acc = acc_ref[h]
        acc_ref[h, :VDIM] = acc[:VDIM] / acc[VDIM : VDIM + 1]
    flat = jnp.concatenate([acc_ref[h, :VDIM] for h in range(qx_ref.shape[0])], 0)
    att[...] = flat.T.astype(jnp.bfloat16)

    def part(owner):
        at = pl.ds(pl.multiple_of(owner * short, short), short)
        return (dot(conv_ref[at, :], cproj_ref[...]) + dot(att[at, :], aproj_ref[...])).astype(jnp.bfloat16)

    tails = []
    for o, mate in enumerate(mates):
        part_buf[o] = part(mate)
        tails.append(
            pltpu.make_async_remote_copy(
                part_buf.at[o],
                in_buf.at[o],
                tail_send.at[o],
                tail_recv.at[o],
                device_id=(me, mate),
                device_id_type=MESH,
            )
        )
        tails[-1].start()
    result = part(t).astype(jnp.float32)
    for o, copy in enumerate(tails):
        copy.wait_recv()
        result = result + in_buf[o].astype(jnp.float32)
    out_ref[...] = result.astype(jnp.bfloat16)
    for copy in tails:
        copy.wait_send()

    @pl.loop(0, z + 1)
    def _(d):
        def sent(j, k):
            for copy in hop(j, k, up):
                copy.wait_send()

        mine = block_of(z - d, 0, 0)

        @pl.when(z + 1 < planes)
        def _():
            sent(mine, 0)

        sent(mine, 1)
        sent(mine, 2)
        sent(block_of(z - d, 1, 0), 2)
        for k in range(4):
            j = block_of(z - d, k % 2, k // 2)

            @pl.when(j < me)
            def _():
                for copy in shares(j):
                    copy.wait_send()


def local(
    tokens,
    outer_gate,
    inner_gate,
    conv_input,
    conv_taps,
    query_down,
    latent_down,
    rotary_down,
    query_gain,
    latent_gain,
    query_up,
    latent_up,
    conv_project,
    attend_project,
):
    rows = tokens.shape[0]
    heads = query_up.shape[1] // (NOPE + ROPE)
    weights = (outer_gate, inner_gate, conv_input, query_down, latent_down, rotary_down)
    piece = lax.all_gather(tokens, "tp", axis=1, tiled=True)
    outer, inner, signal, query_part, latent_part, rotary_raw = tuple(
        (jnp.dot(piece, weight, preferred_element_type=jnp.float32) for weight in weights)
    )
    query_lat = lax.all_gather(query_part.astype(jnp.bfloat16), "tp", axis=1, tiled=True)
    latent_lat = lax.all_gather(latent_part.astype(jnp.bfloat16), "tp", axis=1, tiled=True)
    gated = (inner * signal).astype(jnp.bfloat16)
    reach = conv_taps.shape[0] - 1
    rim = shifted(gated[rows - reach :], "sp", 1)
    padded = jnp.concatenate([rim, gated], 0).astype(jnp.float32)
    taps = conv_taps.astype(jnp.float32)
    filtered = padded[0:rows] * taps[0]
    for index in range(1, reach + 1):
        filtered = filtered + padded[index : index + rows] * taps[index]
    conv_result = (outer * filtered).astype(jnp.bfloat16)
    positions = (lax.axis_index("sp") * rows + jnp.arange(rows, dtype=jnp.int32)).astype(jnp.float32)
    query_norm = rms_scale(query_lat, query_gain)
    latent_norm = rms_scale(latent_lat, latent_gain)
    rotary_key = rotate(rotary_raw, positions).astype(jnp.bfloat16)
    scale = (NOPE + ROPE) ** (-0.5) * log2e
    query = jnp.dot(query_norm, query_up, preferred_element_type=jnp.float32) * scale
    query = query.reshape(rows, heads, NOPE + ROPE)
    plain = query[..., :NOPE].astype(jnp.bfloat16)
    turned = rotate(query[..., NOPE:], positions).astype(jnp.bfloat16)
    qx = jnp.concatenate(
        [
            plain,
            jnp.zeros((rows, heads, VDIM), jnp.bfloat16),
            turned,
            jnp.zeros((rows, heads, LANES - ROPE), jnp.bfloat16),
        ],
        2,
    ).transpose(1, 2, 0)
    kvr = latent_norm.shape[1]
    ways = lax.axis_size("tp")
    blocks = lax.axis_size("sp")
    model = conv_project.shape[1]
    pieces = latent_norm.reshape(rows, ways, kvr // ways).transpose(1, 0, 2)
    wvt = latent_up.reshape(kvr, heads, NOPE + VDIM)[..., NOPE:].reshape(kvr, heads * VDIM).T
    vmem = pl.BlockSpec(memory_space=pltpu.VMEM)
    dma = pltpu.SemaphoreType.DMA
    mates = ways - 1
    return pl.pallas_call(
        mix_kernel,
        out_shape=jax.ShapeDtypeStruct((rows // ways, model), jnp.bfloat16),
        in_specs=[vmem] * 8,
        out_specs=vmem,
        scratch_shapes=[
            pltpu.VMEM((blocks, ways, rows, kvr // ways), jnp.bfloat16),
            pltpu.VMEM((blocks, ROPE, rows), jnp.bfloat16),
            pltpu.VMEM((heads, 1, rows), jnp.float32),
            pltpu.VMEM((heads, VDIM + ONES, rows), jnp.float32),
            pltpu.VMEM((rows, heads * VDIM), jnp.bfloat16),
            pltpu.VMEM((mates, rows // ways, model), jnp.bfloat16),
            pltpu.VMEM((mates, rows // ways, model), jnp.bfloat16),
            dma((2,)),
            dma((blocks, 3)),
            dma((blocks,)),
            dma((blocks, 3)),
            dma((blocks,)),
            dma((blocks, mates)),
            dma((blocks, mates)),
            dma((mates,)),
            dma((mates,)),
        ],
        compiler_params=pltpu.CompilerParams(
            vmem_limit_bytes=56 * 1024 * 1024, collective_id=0, has_side_effects=True
        ),
    )(pieces, rotary_key.T, qx, latent_up, wvt, conv_result, conv_project, attend_project)


def solution(mesh):
    split = P(None, "tp")
    in_specs = (P("sp", "tp"),) + (split,) * 6 + (P(),) * 3 + (split,) * 2 + (P("tp", None),) * 2
    out_specs = P(("sp", "tp"), None)
    return jax.shard_map(local, mesh=mesh, in_specs=in_specs, out_specs=out_specs, check_vma=False)
```

```python
import jax
import jax.numpy as jnp
from jax import lax
from jax.experimental import pallas as pl
from jax.experimental.pallas import tpu as pltpu
from jax.sharding import PartitionSpec as P

NOPE = 64
ROPE = 32
VDIM = 64
LANES = 128
ONES = 16
EDGE = 16

MESH = pl.DeviceIdType.MESH
neg_fill = -1e30
rotary_base = 10000.0
norm_epsilon = 1e-06
log2e = 1.4426950408889634


def dot(a, b, dims=((1,), (0,))):
    return lax.dot_general(a, b, (dims, ((), ())), preferred_element_type=jnp.float32)


def attend(lat, rot, qx_ref, up_ref, wvt_ref, best_ref, acc_ref, masked):
    heads = qx_ref.shape[0]
    expanded = dot(lat, up_ref[...]).astype(jnp.bfloat16)
    turned = dot(wvt_ref[...], lat, ((1,), (1,))).astype(jnp.bfloat16)
    ones = jnp.ones((ONES, lat.shape[0]), jnp.bfloat16)
    width = NOPE + VDIM
    for h in range(heads):
        key = jnp.concatenate([expanded[:, h * width : (h + 1) * width], rot], 1)
        s = dot(key, qx_ref[h])
        if masked:
            k_at = lax.broadcasted_iota(jnp.int32, s.shape, 0)
            q_at = lax.broadcasted_iota(jnp.int32, s.shape, 1)
            s = jnp.where(k_at <= q_at, s, neg_fill)
        values = jnp.concatenate([turned[h * VDIM : (h + 1) * VDIM], ones], 0)
        top = jnp.max(s, 0, keepdims=True)
        if masked:
            weight = jnp.exp2(s - top).astype(jnp.bfloat16)
            acc_ref[h] = dot(values, weight)
            best_ref[h] = top
        else:
            old = best_ref[h]
            new = jnp.maximum(old, top)
            weight = jnp.exp2(s - new).astype(jnp.bfloat16)
            acc_ref[h] = acc_ref[h] * jnp.exp2(old - new) + dot(values, weight)
            best_ref[h] = new


def mix_kernel(
    tok, inv_ref, taps_ref, qgain_ref, lgain_ref,
    ldown_in, qdown_in, rdown_in, inner_in, signal_in, outer_in, qup_in, up_in, cproj_in, aproj_in,
    out_ref,
    ldown, qdown, rdown, inner_w, signal_w, outer_w, qup, up_ref, cproj_ref, aproj_ref,
    xbuf, raw_lat, raw_query, edge, rim, padded, conv_ref, wvt_ref, qx_ref,
    lat, rot, best_ref, acc_ref, att, part_buf, in_buf,
    load_sem, front_send, front_recv, lat_send, lat_recv, rot_send, rot_recv, share_send, share_recv, tail_send, tail_recv,
):
    me = lax.axis_index("sp")
    t = lax.axis_index("tp")
    total = lax.axis_size("sp")
    ways = lax.axis_size("tp")
    planes = total // 4
    z = me // 4
    b0 = me % 2
    b1 = (me // 2) % 2
    a0 = 1 - t % 2
    rows = qx_ref.shape[2]
    short = rows // ways

    def block_of(plane, ka, kb):
        f0 = a0 * ka + (1 - a0) * kb
        f1 = a0 * kb + (1 - a0) * ka
        return plane * 4 + (b1 + f1 * (1 - 2 * b1)) * 2 + b0 + f0 * (1 - 2 * b0)

    up = lax.rem(me + 4, total)
    down = lax.rem(me + total - 4, total)
    after = lax.rem(me + 1, total)
    before = lax.rem(me + total - 1, total)
    a_peer = block_of(z, 1, 0)
    b_peer = block_of(z, 0, 1)
    mates = [lax.rem(t + o, ways) for o in range(1, ways)]

    barrier = pltpu.get_barrier_semaphore()
    for target in [(up, t), (down, t), (a_peer, t), (b_peer, t), (after, t), (before, t)] + [(me, mate) for mate in mates]:
        pl.semaphore_signal(barrier, inc=1, device_id=target, device_id_type=MESH)

    pairs = (
        (ldown_in, ldown), (qdown_in, qdown), (rdown_in, rdown), (inner_in, inner_w), (signal_in, signal_w),
        (outer_in, outer_w), (qup_in, qup), (up_in, up_ref), (cproj_in, cproj_ref), (aproj_in, aproj_ref),
    )
    loads = [pltpu.make_async_copy(a, b, load_sem.at[i]) for i, (a, b) in enumerate(pairs)]
    for copy in loads:
        copy.start()
    pl.semaphore_wait(barrier, 6 + len(mates))

    def to_mates(source, slots, kind):
        return [
            pltpu.make_async_remote_copy(
                source, slots.at[o], front_send.at[kind, o], front_recv.at[kind, o],
                device_id=(me, mate), device_id_type=MESH,
            )
            for o, mate in enumerate(mates)
        ]

    token_sends = to_mates(tok, xbuf, 0)
    for copy in token_sends:
        copy.start()
    depth = tok.shape[1]

    def rows_from(weight, o):
        at = pl.multiple_of(lax.rem(t + ways - o, ways) * depth, depth)
        return weight[pl.ds(at, depth), :]

    def rest(value, weight):
        for o in range(1, ways):
            value = value + dot(xbuf[o - 1], rows_from(weight, o))
        return value

    for copy in loads[:3]:
        copy.wait()
    first = [dot(tok[...], rows_from(weight, 0)) for weight in (ldown, qdown, rdown)]
    for copy in token_sends:
        copy.wait_recv()
    lat_part, query_part, turn_part = [rest(v, w) for v, w in zip(first, (ldown, qdown, rdown))]
    raw_lat[ways - 1] = lat_part.astype(jnp.bfloat16)
    raw_query[ways - 1] = query_part.astype(jnp.bfloat16)
    latent_sends = to_mates(raw_lat.at[ways - 1], raw_lat, 1) + to_mates(raw_query.at[ways - 1], raw_query, 2)
    for copy in latent_sends:
        copy.start()

    position = (me * rows + lax.broadcasted_iota(jnp.int32, (1, rows), 1)).astype(jnp.float32)
    angle = inv_ref[...] * position
    cosine = jnp.cos(angle)
    sine = jnp.sin(angle)
    half = ROPE // 2

    def rotated(values):
        a = values[:half]
        b = values[half:]
        return jnp.concatenate([a * cosine - b * sine, a * sine + b * cosine], 0).astype(jnp.bfloat16)

    turn = jnp.concatenate([turn_part, jnp.zeros((rows, LANES - ROPE), jnp.float32)], 1).T
    rot[me] = rotated(turn[:ROPE])

    loads[3].wait()
    loads[4].wait()
    inner = rest(dot(tok[...], rows_from(inner_w, 0)), inner_w)
    signal = rest(dot(tok[...], rows_from(signal_w, 0)), signal_w)
    gated = (inner * signal).astype(jnp.bfloat16)
    padded[EDGE:] = gated.astype(jnp.float32)
    edge[...] = gated[rows - EDGE :]

    def whole(raw, gain_ref):
        values = jnp.concatenate([raw[lax.rem(t + ways - 1 - s, ways)] for s in range(ways)], 1).astype(jnp.float32)
        factor = lax.rsqrt(jnp.mean(values * values, -1, keepdims=True) + norm_epsilon)
        return (values * factor * gain_ref[...]).astype(jnp.bfloat16)

    for copy in latent_sends:
        copy.wait_recv()
    latent_norm = whole(raw_lat, lgain_ref)
    wide = latent_norm.shape[1] // ways
    for s in range(ways):
        lat[me, s] = latent_norm[:, s * wide : (s + 1) * wide]

    def hop(j, k, target):
        return [
            pltpu.make_async_remote_copy(
                buf.at[j, t] if split else buf.at[j],
                buf.at[j, t] if split else buf.at[j],
                send.at[j, k],
                recv.at[j],
                device_id=(target, t),
                device_id_type=MESH,
            )
            for buf, send, recv, split in ((lat, lat_send, lat_recv, True), (rot, rot_send, rot_recv, False))
        ]

    def start(j, k, target):
        for copy in hop(j, k, target):
            copy.start()

    def arrive(j):
        for copy in hop(j, 0, up):
            copy.wait_recv()

    def shares(j):
        return [
            pltpu.make_async_remote_copy(
                lat.at[j, t],
                lat.at[j, t],
                share_send.at[j, o],
                share_recv.at[j, o],
                device_id=(me, mate),
                device_id_type=MESH,
            )
            for o, mate in enumerate(mates)
        ]

    def share_landed(j):
        for o in range(len(mates)):
            source = lax.rem(t + ways - 1 - o, ways)
            pltpu.make_async_remote_copy(
                lat.at[j, source],
                lat.at[j, source],
                share_send.at[j, o],
                share_recv.at[j, o],
                device_id=(me, mates[o]),
                device_id_type=MESH,
            ).wait_recv()

    def share(j):
        @pl.when(j < me)
        def _():
            for copy in shares(j):
                copy.start()

    def spread(j):
        @pl.when(z + 1 < planes)
        def _():
            start(j, 0, up)

        start(j, 1, a_peer)
        start(j, 2, b_peer)

    def stage_a(d):
        j = block_of(z - d, 0, 0)
        arrive(j)
        spread(j)
        share(j)

    def stage_b(d):
        j = block_of(z - d, 1, 0)
        arrive(j)
        start(j, 2, b_peer)
        share(j)

    def stage_c(d):
        for ka in (0, 1):
            j = block_of(z - d, ka, 1)
            arrive(j)
            share(j)

    def block(j, masked):
        latent = jnp.concatenate([lat[j, s] for s in range(ways)], 1)
        turned = rot[j].astype(jnp.float32)
        turned = jnp.concatenate([turned, jnp.zeros((LANES - ROPE, rows), jnp.float32)], 0)
        turned = turned.T.astype(jnp.bfloat16)
        attend(latent, turned, qx_ref, up_ref, wvt_ref, best_ref, acc_ref, masked)

    spread(me)
    rim_copy = pltpu.make_async_remote_copy(
        edge, rim, front_send.at[3, 0], front_recv.at[3, 0], device_id=(after, t), device_id_type=MESH
    )

    @pl.when(me + 1 < total)
    def _():
        rim_copy.start()

    loads[6].wait()
    loads[7].wait()
    scale = (NOPE + ROPE) ** (-0.5) * log2e
    query = (dot(whole(raw_query, qgain_ref), qup[...]) * scale).T
    heads = qx_ref.shape[0]
    size = NOPE + ROPE
    turned_up = up_ref[...].astype(jnp.float32).T.astype(jnp.bfloat16)
    for h in range(heads):
        base = h * size
        qx_ref[h, :NOPE] = query[base : base + NOPE].astype(jnp.bfloat16)
        qx_ref[h, NOPE : NOPE + VDIM] = jnp.zeros((VDIM, rows), jnp.bfloat16)
        qx_ref[h, NOPE + VDIM : NOPE + VDIM + ROPE] = rotated(query[base + NOPE : base + size])
        qx_ref[h, NOPE + VDIM + ROPE :] = jnp.zeros((LANES - ROPE, rows), jnp.bfloat16)
        low = h * (NOPE + VDIM) + NOPE
        wvt_ref[h * VDIM : (h + 1) * VDIM] = turned_up[low : low + VDIM]

    block(me, True)
    stage_b(0)
    loads[5].wait()
    outer = rest(dot(tok[...], rows_from(outer_w, 0)), outer_w)

    @pl.when(me > 0)
    def _():
        rim_copy.wait_recv()
        padded[:EDGE] = rim[...].astype(jnp.float32)

    @pl.when(me == 0)
    def _():
        padded[:EDGE] = jnp.zeros((EDGE, padded.shape[1]), jnp.float32)

    reach = taps_ref.shape[0] - 1
    filtered = padded[EDGE:] * taps_ref[reach : reach + 1, :]
    for k in range(reach):
        filtered = filtered + padded[EDGE - reach + k : EDGE - reach + k + rows] * taps_ref[k : k + 1, :]
    conv_ref[...] = (outer * filtered).astype(jnp.bfloat16)
    stage_c(0)

    @pl.loop(0, 4 * (z + 1))
    def _(n):
        d = n // 4
        k = n % 4
        for order, stage in enumerate((stage_a, stage_b, stage_c)):

            @pl.when(jnp.logical_and(k == order, d < z))
            def _():
                stage(d + 1)

        j = block_of(z - d, k % 2, k // 2)

        @pl.when(j < me)
        def _():
            share_landed(j)
            block(j, False)

    for h in range(qx_ref.shape[0]):
        acc = acc_ref[h]
        acc_ref[h, :VDIM] = acc[:VDIM] / acc[VDIM : VDIM + 1]
    flat = jnp.concatenate([acc_ref[h, :VDIM] for h in range(qx_ref.shape[0])], 0)
    att[...] = flat.T.astype(jnp.bfloat16)

    loads[8].wait()
    loads[9].wait()

    def part(owner):
        at = pl.ds(pl.multiple_of(owner * short, short), short)
        return (dot(conv_ref[at, :], cproj_ref[...]) + dot(att[at, :], aproj_ref[...])).astype(jnp.bfloat16)

    tails = []
    for o, mate in enumerate(mates):
        part_buf[o] = part(mate)
        tails.append(
            pltpu.make_async_remote_copy(
                part_buf.at[o],
                in_buf.at[o],
                tail_send.at[o],
                tail_recv.at[o],
                device_id=(me, mate),
                device_id_type=MESH,
            )
        )
        tails[-1].start()
    result = part(t).astype(jnp.float32)
    for o, copy in enumerate(tails):
        copy.wait_recv()
        result = result + in_buf[o].astype(jnp.float32)
    out_ref[...] = result.astype(jnp.bfloat16)
    for copy in tails + token_sends + latent_sends:
        copy.wait_send()

    @pl.when(me + 1 < total)
    def _():
        rim_copy.wait_send()

    @pl.loop(0, z + 1)
    def _(d):
        def sent(j, k):
            for copy in hop(j, k, up):
                copy.wait_send()

        mine = block_of(z - d, 0, 0)

        @pl.when(z + 1 < planes)
        def _():
            sent(mine, 0)

        sent(mine, 1)
        sent(mine, 2)
        sent(block_of(z - d, 1, 0), 2)
        for k in range(4):
            j = block_of(z - d, k % 2, k // 2)

            @pl.when(j < me)
            def _():
                for copy in shares(j):
                    copy.wait_send()


def local(
    tokens,
    outer_gate,
    inner_gate,
    conv_input,
    conv_taps,
    query_down,
    latent_down,
    rotary_down,
    query_gain,
    latent_gain,
    query_up,
    latent_up,
    conv_project,
    attend_project,
):
    rows = tokens.shape[0]
    heads = query_up.shape[1] // (NOPE + ROPE)
    ways = lax.axis_size("tp")
    blocks = lax.axis_size("sp")
    model = conv_project.shape[1]
    kvr = latent_up.shape[0]
    channels = conv_project.shape[0]
    half = ROPE // 2
    inverse = rotary_base ** (-(jnp.arange(half, dtype=jnp.float32) * 2.0 / (2 * half)))
    vmem = pl.BlockSpec(memory_space=pltpu.VMEM)
    dma = pltpu.SemaphoreType.DMA
    mates = ways - 1
    big = (
        latent_down, query_down, rotary_down, inner_gate, conv_input,
        outer_gate, query_up, latent_up, conv_project, attend_project,
    )

    def half_type(*shape):
        return pltpu.VMEM(shape, jnp.bfloat16)

    def full_type(*shape):
        return pltpu.VMEM(shape, jnp.float32)

    return pl.pallas_call(
        mix_kernel,
        out_shape=jax.ShapeDtypeStruct((rows // ways, model), jnp.bfloat16),
        in_specs=[vmem] * 5 + [pl.BlockSpec(memory_space=pl.ANY)] * len(big),
        out_specs=vmem,
        scratch_shapes=[half_type(*array.shape) for array in big]
        + [
            half_type(mates, *tokens.shape),
            half_type(ways, rows, latent_down.shape[1]),
            half_type(ways, rows, query_down.shape[1]),
            half_type(EDGE, channels),
            half_type(EDGE, channels),
            full_type(EDGE + rows, channels),
            half_type(rows, channels),
            half_type(heads * VDIM, kvr),
            half_type(heads, NOPE + VDIM + LANES, rows),
            half_type(blocks, ways, rows, kvr // ways),
            half_type(blocks, ROPE, rows),
            full_type(heads, 1, rows),
            full_type(heads, VDIM + ONES, rows),
            half_type(rows, heads * VDIM),
            half_type(mates, rows // ways, model),
            half_type(mates, rows // ways, model),
            dma((len(big),)),
            dma((4, mates)),
            dma((4, mates)),
            dma((blocks, 3)),
            dma((blocks,)),
            dma((blocks, 3)),
            dma((blocks,)),
            dma((blocks, mates)),
            dma((blocks, mates)),
            dma((mates,)),
            dma((mates,)),
        ],
        compiler_params=pltpu.CompilerParams(
            vmem_limit_bytes=60 * 1024 * 1024, collective_id=0, has_side_effects=True
        ),
    )(
        tokens,
        inverse[:, None],
        conv_taps.astype(jnp.float32),
        query_gain[None, :],
        latent_gain[None, :],
        *big,
    )


def solution(mesh):
    split = P(None, "tp")
    in_specs = (P("sp", "tp"),) + (split,) * 6 + (P(),) * 3 + (split,) * 2 + (P("tp", None),) * 2
    out_specs = P(("sp", "tp"), None)
    return jax.shard_map(local, mesh=mesh, in_specs=in_specs, out_specs=out_specs, check_vma=False)
```

```python
import jax
import numpy as np
import jax.numpy as jnp
from jax import lax
from jax.experimental import pallas as pl
from jax.experimental.pallas import tpu as pltpu
from jax.sharding import PartitionSpec as P

NOPE = 64
ROPE = 32
VDIM = 64
LANES = 128
ONES = 16
EDGE = 16

MESH = pl.DeviceIdType.MESH
neg_fill = -1e30
rotary_base = 10000.0
norm_epsilon = 1e-06
log2e = 1.4426950408889634


def dot(a, b, dims=((1,), (0,))):
    return lax.dot_general(a, b, (dims, ((), ())), preferred_element_type=jnp.float32)


def attend(lat, rot, qx_ref, up_ref, wvt_ref, best_ref, acc_ref, masked):
    heads = qx_ref.shape[0]
    expanded = dot(lat, up_ref[...]).astype(jnp.bfloat16)
    turned = dot(wvt_ref[...], lat, ((1,), (1,))).astype(jnp.bfloat16)
    ones = jnp.ones((ONES, lat.shape[0]), jnp.bfloat16)
    width = NOPE + VDIM
    for h in range(heads):
        key = jnp.concatenate([expanded[:, h * width : (h + 1) * width], rot], 1)
        s = dot(key, qx_ref[h])
        if masked:
            k_at = lax.broadcasted_iota(jnp.int32, s.shape, 0)
            q_at = lax.broadcasted_iota(jnp.int32, s.shape, 1)
            s = jnp.where(k_at <= q_at, s, neg_fill)
        values = jnp.concatenate([turned[h * VDIM : (h + 1) * VDIM], ones], 0)
        top = jnp.max(s, 0, keepdims=True)
        if masked:
            weight = jnp.exp2((s - top).astype(jnp.bfloat16))
            acc_ref[h] = dot(values, weight)
            best_ref[h] = top
        else:
            old = best_ref[h]
            new = jnp.maximum(old, top)
            weight = jnp.exp2((s - new).astype(jnp.bfloat16))
            acc_ref[h] = acc_ref[h] * jnp.exp2(old - new) + dot(values, weight)
            best_ref[h] = new


def mix_kernel(
    tok, inv_ref, taps_ref, qgain_ref, lgain_ref,
    ldown_in, qdown_in, rdown_in, inner_in, signal_in, outer_in, qup_in, up_in, cproj_in, aproj_in,
    out_ref,
    ldown, qdown, rdown, inner_w, signal_w, outer_w, qup, up_ref, cproj_ref, aproj_ref,
    xbuf, raw_lat, raw_query, edge, rim, padded, conv_ref, wvt_ref, qx_ref,
    lat, rot, best_ref, acc_ref, att, part_buf, in_buf,
    load_sem, front_send, front_recv, lat_send, lat_recv, rot_send, rot_recv, share_send, share_recv, tail_send, tail_recv,
):
    me = lax.axis_index("sp")
    t = lax.axis_index("tp")
    total = lax.axis_size("sp")
    ways = lax.axis_size("tp")
    planes = total // 4
    z = me // 4
    b0 = me % 2
    b1 = (me // 2) % 2
    a0 = 1 - t % 2
    rows = qx_ref.shape[2]
    short = rows // ways

    def block_of(plane, ka, kb):
        f0 = a0 * ka + (1 - a0) * kb
        f1 = a0 * kb + (1 - a0) * ka
        return plane * 4 + (b1 + f1 * (1 - 2 * b1)) * 2 + b0 + f0 * (1 - 2 * b0)

    up = lax.rem(me + 4, total)
    down = lax.rem(me + total - 4, total)
    after = lax.rem(me + 1, total)
    before = lax.rem(me + total - 1, total)
    a_peer = block_of(z, 1, 0)
    b_peer = block_of(z, 0, 1)
    mates = [lax.rem(t + o, ways) for o in range(1, ways)]

    barrier = pltpu.get_barrier_semaphore()
    for target in [(up, t), (down, t), (a_peer, t), (b_peer, t), (after, t), (before, t)] + [(me, mate) for mate in mates]:
        pl.semaphore_signal(barrier, inc=1, device_id=target, device_id_type=MESH)

    pairs = (
        (ldown_in, ldown), (qdown_in, qdown), (rdown_in, rdown), (inner_in, inner_w), (signal_in, signal_w),
        (outer_in, outer_w), (qup_in, qup), (up_in, up_ref), (cproj_in, cproj_ref), (aproj_in, aproj_ref),
    )
    loads = [pltpu.make_async_copy(a, b, load_sem.at[i]) for i, (a, b) in enumerate(pairs)]
    for copy in loads:
        copy.start()
    pl.semaphore_wait(barrier, 6 + len(mates))

    def to_mates(source, slots, kind):
        return [
            pltpu.make_async_remote_copy(
                source, slots.at[o], front_send.at[kind, o], front_recv.at[kind, o],
                device_id=(me, mate), device_id_type=MESH,
            )
            for o, mate in enumerate(mates)
        ]

    token_sends = to_mates(tok, xbuf, 0)
    for copy in token_sends:
        copy.start()
    depth = tok.shape[1]

    def rows_from(weight, o):
        at = pl.multiple_of(lax.rem(t + ways - o, ways) * depth, depth)
        if weight is rdown:
            return weight[:, pl.ds(at, depth)]
        return weight[pl.ds(at, depth), :]

    def project(x, weight, o):
        return dot(x, rows_from(weight, o), ((1,), (1 if weight is rdown else 0,)))

    def rest(value, weight):
        for o in range(1, ways):
            value = value + project(xbuf[o - 1], weight, o)
        return value

    for copy in loads[:3]:
        copy.wait()
    first = [project(tok[...], weight, 0) for weight in (ldown, qdown, rdown)]
    for copy in token_sends:
        copy.wait_recv()
    lat_part, query_part, turn_part = [rest(v, w) for v, w in zip(first, (ldown, qdown, rdown))]
    raw_lat[ways - 1] = lat_part.astype(jnp.bfloat16)
    raw_query[ways - 1] = query_part.astype(jnp.bfloat16)
    latent_sends = to_mates(raw_lat.at[ways - 1], raw_lat, 1) + to_mates(raw_query.at[ways - 1], raw_query, 2)
    for copy in latent_sends:
        copy.start()

    position = (me * rows + lax.broadcasted_iota(jnp.int32, (1, rows), 1)).astype(jnp.float32)
    angle = inv_ref[...] * position
    cosine = jnp.cos(angle)
    sine = jnp.sin(angle)
    half = ROPE // 2

    def rotated(values):
        a = values[:half]
        b = values[half:]
        return jnp.concatenate([a * cosine - b * sine, a * sine + b * cosine], 0).astype(jnp.bfloat16)

    turn = jnp.concatenate([turn_part, jnp.zeros((rows, LANES - ROPE), jnp.float32)], 1).T
    rot[me] = rotated(turn[:ROPE])

    loads[3].wait()
    loads[4].wait()
    inner = rest(dot(tok[...], rows_from(inner_w, 0)), inner_w)
    signal = rest(dot(tok[...], rows_from(signal_w, 0)), signal_w)
    gated = (inner * signal).astype(jnp.bfloat16)
    padded[EDGE:] = gated.astype(jnp.float32)
    edge[...] = gated[rows - EDGE :]

    def whole(raw, gain_ref):
        values = jnp.concatenate([raw[lax.rem(t + ways - 1 - s, ways)] for s in range(ways)], 1).astype(jnp.float32)
        factor = lax.rsqrt(jnp.mean(values * values, -1, keepdims=True) + norm_epsilon)
        return (values * factor * gain_ref[...]).astype(jnp.bfloat16)

    for copy in latent_sends:
        copy.wait_recv()
    latent_norm = whole(raw_lat, lgain_ref)
    wide = latent_norm.shape[1] // ways
    for s in range(ways):
        lat[me, s] = latent_norm[:, s * wide : (s + 1) * wide]

    def hop(j, k, target):
        return [
            pltpu.make_async_remote_copy(
                buf.at[j, t] if split else buf.at[j],
                buf.at[j, t] if split else buf.at[j],
                send.at[j, k],
                recv.at[j],
                device_id=(target, t),
                device_id_type=MESH,
            )
            for buf, send, recv, split in ((lat, lat_send, lat_recv, True), (rot, rot_send, rot_recv, False))
        ]

    def start(j, k, target):
        for copy in hop(j, k, target):
            copy.start()

    def arrive(j):
        for copy in hop(j, 0, up):
            copy.wait_recv()

    def shares(j):
        return [
            pltpu.make_async_remote_copy(
                lat.at[j, t],
                lat.at[j, t],
                share_send.at[j, o],
                share_recv.at[j, o],
                device_id=(me, mate),
                device_id_type=MESH,
            )
            for o, mate in enumerate(mates)
        ]

    def share_landed(j):
        for o in range(len(mates)):
            source = lax.rem(t + ways - 1 - o, ways)
            pltpu.make_async_remote_copy(
                lat.at[j, source],
                lat.at[j, source],
                share_send.at[j, o],
                share_recv.at[j, o],
                device_id=(me, mates[o]),
                device_id_type=MESH,
            ).wait_recv()

    def share(j):
        @pl.when(j < me)
        def _():
            for copy in shares(j):
                copy.start()

    def spread(j):
        @pl.when(z + 1 < planes)
        def _():
            start(j, 0, up)

        start(j, 1, a_peer)
        start(j, 2, b_peer)

    def stage_a(d):
        j = block_of(z - d, 0, 0)
        arrive(j)
        spread(j)
        share(j)

    def stage_b(d):
        j = block_of(z - d, 1, 0)
        arrive(j)
        start(j, 2, b_peer)
        share(j)

    def stage_c(d):
        for ka in (0, 1):
            j = block_of(z - d, ka, 1)
            arrive(j)
            share(j)

    def block(j, masked):
        latent = jnp.concatenate([lat[j, s] for s in range(ways)], 1)
        turned = rot[j].astype(jnp.float32)
        turned = jnp.concatenate([turned, jnp.zeros((LANES - ROPE, rows), jnp.float32)], 0)
        turned = turned.T.astype(jnp.bfloat16)
        attend(latent, turned, qx_ref, up_ref, wvt_ref, best_ref, acc_ref, masked)

    spread(me)
    rim_copy = pltpu.make_async_remote_copy(
        edge, rim, front_send.at[3, 0], front_recv.at[3, 0], device_id=(after, t), device_id_type=MESH
    )

    @pl.when(me + 1 < total)
    def _():
        rim_copy.start()

    loads[6].wait()
    loads[7].wait()
    scale = (NOPE + ROPE) ** (-0.5) * log2e
    query = (dot(whole(raw_query, qgain_ref), qup[...]) * scale).T
    heads = qx_ref.shape[0]
    size = NOPE + ROPE
    turned_up = up_ref[...].astype(jnp.float32).T.astype(jnp.bfloat16)
    for h in range(heads):
        base = h * size
        qx_ref[h, :NOPE] = query[base : base + NOPE].astype(jnp.bfloat16)
        qx_ref[h, NOPE : NOPE + VDIM] = jnp.zeros((VDIM, rows), jnp.bfloat16)
        qx_ref[h, NOPE + VDIM : NOPE + VDIM + ROPE] = rotated(query[base + NOPE : base + size])
        qx_ref[h, NOPE + VDIM + ROPE :] = jnp.zeros((LANES - ROPE, rows), jnp.bfloat16)
        low = h * (NOPE + VDIM) + NOPE
        wvt_ref[h * VDIM : (h + 1) * VDIM] = turned_up[low : low + VDIM]

    block(me, True)
    stage_b(0)
    loads[5].wait()
    outer = rest(dot(tok[...], rows_from(outer_w, 0)), outer_w)

    @pl.when(me > 0)
    def _():
        rim_copy.wait_recv()
        padded[:EDGE] = rim[...].astype(jnp.float32)

    @pl.when(me == 0)
    def _():
        padded[:EDGE] = jnp.zeros((EDGE, padded.shape[1]), jnp.float32)

    reach = taps_ref.shape[0] - 1
    taps = taps_ref[...].astype(jnp.float32)
    filtered = padded[EDGE:] * taps[reach : reach + 1, :]
    for k in range(reach):
        filtered = filtered + padded[EDGE - reach + k : EDGE - reach + k + rows] * taps[k : k + 1, :]
    conv_ref[...] = (outer * filtered).astype(jnp.bfloat16)
    stage_c(0)

    @pl.loop(0, 4 * (z + 1))
    def _(n):
        d = n // 4
        k = n % 4
        for order, stage in enumerate((stage_a, stage_b, stage_c)):

            @pl.when(jnp.logical_and(k == order, d < z))
            def _():
                stage(d + 1)

        j = block_of(z - d, k % 2, k // 2)

        @pl.when(j < me)
        def _():
            share_landed(j)
            block(j, False)

    for h in range(qx_ref.shape[0]):
        acc = acc_ref[h]
        acc_ref[h, :VDIM] = acc[:VDIM] / acc[VDIM : VDIM + 1]
    flat = jnp.concatenate([acc_ref[h, :VDIM] for h in range(qx_ref.shape[0])], 0)
    att[...] = flat.T.astype(jnp.bfloat16)

    loads[8].wait()
    loads[9].wait()

    def part(owner):
        at = pl.ds(pl.multiple_of(owner * short, short), short)
        return (dot(conv_ref[at, :], cproj_ref[...]) + dot(att[at, :], aproj_ref[...])).astype(jnp.bfloat16)

    tails = []
    for o, mate in enumerate(mates):
        part_buf[o] = part(mate)
        tails.append(
            pltpu.make_async_remote_copy(
                part_buf.at[o],
                in_buf.at[o],
                tail_send.at[o],
                tail_recv.at[o],
                device_id=(me, mate),
                device_id_type=MESH,
            )
        )
        tails[-1].start()
    result = part(t).astype(jnp.float32)
    for o, copy in enumerate(tails):
        copy.wait_recv()
        result = result + in_buf[o].astype(jnp.float32)
    out_ref[...] = result.astype(jnp.bfloat16)
    for copy in tails + token_sends + latent_sends:
        copy.wait_send()

    @pl.when(me + 1 < total)
    def _():
        rim_copy.wait_send()

    @pl.loop(0, z + 1)
    def _(d):
        def sent(j, k):
            for copy in hop(j, k, up):
                copy.wait_send()

        mine = block_of(z - d, 0, 0)

        @pl.when(z + 1 < planes)
        def _():
            sent(mine, 0)

        sent(mine, 1)
        sent(mine, 2)
        sent(block_of(z - d, 1, 0), 2)
        for k in range(4):
            j = block_of(z - d, k % 2, k // 2)

            @pl.when(j < me)
            def _():
                for copy in shares(j):
                    copy.wait_send()


def local(
    tokens,
    outer_gate,
    inner_gate,
    conv_input,
    conv_taps,
    query_down,
    latent_down,
    rotary_down,
    query_gain,
    latent_gain,
    query_up,
    latent_up,
    conv_project,
    attend_project,
):
    rows = tokens.shape[0]
    heads = query_up.shape[1] // (NOPE + ROPE)
    ways = lax.axis_size("tp")
    blocks = lax.axis_size("sp")
    model = conv_project.shape[1]
    kvr = latent_up.shape[0]
    channels = conv_project.shape[0]
    half = ROPE // 2
    inverse = jnp.asarray(np.float32(rotary_base) ** (-(np.arange(half, dtype=np.float32) * 2.0 / (2 * half))), jnp.float32)
    vmem = pl.BlockSpec(memory_space=pltpu.VMEM)
    dma = pltpu.SemaphoreType.DMA
    mates = ways - 1
    big = (
        latent_down, query_down, rotary_down.T, inner_gate, conv_input,
        outer_gate, query_up, latent_up, conv_project, attend_project,
    )

    def half_type(*shape):
        return pltpu.VMEM(shape, jnp.bfloat16)

    def full_type(*shape):
        return pltpu.VMEM(shape, jnp.float32)

    return pl.pallas_call(
        mix_kernel,
        out_shape=jax.ShapeDtypeStruct((rows // ways, model), jnp.bfloat16),
        in_specs=[vmem] * 5 + [pl.BlockSpec(memory_space=pl.ANY)] * len(big),
        out_specs=vmem,
        scratch_shapes=[half_type(*array.shape) for array in big]
        + [
            half_type(mates, *tokens.shape),
            half_type(ways, rows, latent_down.shape[1]),
            half_type(ways, rows, query_down.shape[1]),
            half_type(EDGE, channels),
            half_type(EDGE, channels),
            full_type(EDGE + rows, channels),
            half_type(rows, channels),
            half_type(heads * VDIM, kvr),
            half_type(heads, NOPE + VDIM + LANES, rows),
            half_type(blocks, ways, rows, kvr // ways),
            half_type(blocks, ROPE, rows),
            full_type(heads, 1, rows),
            full_type(heads, VDIM + ONES, rows),
            half_type(rows, heads * VDIM),
            half_type(mates, rows // ways, model),
            half_type(mates, rows // ways, model),
            dma((len(big),)),
            dma((4, mates)),
            dma((4, mates)),
            dma((blocks, 3)),
            dma((blocks,)),
            dma((blocks, 3)),
            dma((blocks,)),
            dma((blocks, mates)),
            dma((blocks, mates)),
            dma((mates,)),
            dma((mates,)),
        ],
        compiler_params=pltpu.CompilerParams(
            vmem_limit_bytes=60 * 1024 * 1024, collective_id=0, has_side_effects=True
        ),
    )(
        tokens,
        inverse[:, None],
        conv_taps,
        query_gain[None, :],
        latent_gain[None, :],
        *big,
    )


def solution(mesh):
    split = P(None, "tp")
    in_specs = (P("sp", "tp"),) + (split,) * 6 + (P(),) * 3 + (split,) * 2 + (P("tp", None),) * 2
    out_specs = P(("sp", "tp"), None)
    return jax.shard_map(local, mesh=mesh, in_specs=in_specs, out_specs=out_specs, check_vma=False)
```
